1024 devices in a mesh: row: 64 (over z, y), col: 16 (over x, core).
Axes of the slice: x: 8, y: 8, z: 8, core: 2. Of those that a mesh axis runs over, the one named last changes fastest.
Arguments:
- tokens: bfloat16 [2, 256, 64, 2048], P(None, 'row', 'col'), may hold values from -6 to 6
- norm_gain: bfloat16 [2048], replicated, may hold values from 0.099609375 to 1.8984375
- w_mix_in: bfloat16 [2048, 1024], replicated, may hold values from -0.125 to 0.125
- w_mix_out: bfloat16 [1024, 2048], replicated, may hold values from -0.1875 to 0.1875
Outputs:
- mixed_tokens: bfloat16 [2, 64, 256, 2048], P(None, 'row', 'col')
The draws below stay inside these ranges and needn't reach their ends.
All inputs are finite; a program needn't handle non-finite values.
Results may differ from the reference program's by a relative error of at most 0.013.
Values may be sent and summed in bfloat16 or wider, within the bound.
No kernel may reach another device: no remote copies, remote signals or barrier semaphores. Data moves between devices by JAX's collectives and lax.ppermute only.
A program may use at most 32 MiB of HBM per device.

```python
import jax
import jax.numpy as jnp
from jax import lax

D = 2048
F = 1024
G = 128
SEQS = 2
LEN_ROW = 256
LEN_COL = 64


def block_scale(own_key, shape, cuts, low, largest):
    def one(position, shards_of):
        heights = jax.random.uniform(jax.random.fold_in(jax.random.fold_in(own_key, 6), position), (shards_of,), jnp.float32, low / len(cuts), largest / len(cuts))
        return jnp.repeat(jnp.exp(heights), shape[position] // shards_of).reshape((-1,) + (1,) * (len(shape) - position - 1))

    level = one(*cuts[0])
    for cut in cuts[1:]:
        level = level * one(*cut)
    return level


def gaussian(key, extent, width, limit, cuts=(), kind=jnp.bfloat16):
    array = width * jax.random.normal(key, extent, jnp.float32)
    if cuts:
        array = array * block_scale(key, extent, cuts, -0.22, 0.18)
    return jnp.clip(array, -limit, limit).astype(kind)


def setup_inputs(seed: int = 0) -> dict:
    streams_of = jax.random.split(jax.random.key(seed), 5)
    return {
        "tokens": gaussian(streams_of[0], (SEQS, LEN_ROW, LEN_COL, D), 1.0, 6.0, ((1, 64), (2, 16))),
        "norm_gain": jnp.clip(1.0 + 0.18 * jax.random.normal(streams_of[1], (D,), jnp.float32), 0.099609375, 1.8984375).astype(jnp.bfloat16),
        "w_mix_in": gaussian(streams_of[2], (D, F), D ** -0.5, 0.125),
        "w_mix_out": gaussian(streams_of[3], (F, D), F ** -0.5, 0.1875),
    }


EPS = 1e-06

def reference(tokens, norm_gain, w_mix_in, w_mix_out):

    def one_sequence(sequence):
        scaled = sequence.astype(jnp.float32)
        mean_square = lax.optimization_barrier(jnp.mean(scaled * scaled, axis=-1, keepdims=True))
        normed = (scaled * lax.rsqrt(mean_square + EPS) * norm_gain.astype(jnp.float32)).astype(jnp.bfloat16)
        mixing_in = jnp.dot(normed.reshape(LEN_ROW * LEN_COL, D), w_mix_in, preferred_element_type=jnp.float32).astype(jnp.bfloat16)
        grouped = mixing_in.astype(jnp.float32).reshape(LEN_ROW * LEN_COL, F // G, G)
        spectrum = jnp.fft.fft2(grouped, axes=(0, 2), norm='ortho').real
        mixed = spectrum.astype(jnp.bfloat16).reshape(LEN_COL * LEN_ROW, F)
        output = jnp.dot(mixed, w_mix_out, preferred_element_type=jnp.float32).astype(jnp.bfloat16)
        return output.reshape(LEN_COL, LEN_ROW, D)
    return lax.map(one_sequence, tokens)
```

```python
import math

import jax
import jax.numpy as jnp
import numpy as np
from jax import lax
from jax.experimental import pallas as pl
from jax.experimental.pallas import tpu as pltpu
from jax.sharding import PartitionSpec as P

D = 2048
F = 1024
G = 128
GROUPS = F // G
SEQS = 2
ROW = 64
COL = 16
A = 4
B = 4
LEN1 = ROW * A
LEN2 = COL * B
LENGTH = LEN1 * LEN2
EPS = 1e-06
IN_CHUNKS = 4
OUT_CHUNKS = 8
bf16 = jnp.bfloat16
f32 = jnp.float32


def channel_table():
    c = np.arange(G)[None, :]
    r = np.arange(ROW)[:, None]
    cos = np.cos(2 * np.pi * (c * r % G) / G)
    sin = np.sin(2 * np.pi * (c * r % G) / G)
    sin[0] = np.cos(np.pi * np.arange(G))
    return np.concatenate([cos, sin], 0)


def first_tables():
    k1 = np.arange(LEN1)[:, None]
    phase = 2 * np.pi * (k1 * np.arange(LEN1)[None, :] % LEN1) / LEN1
    re, im = np.cos(phase) / math.sqrt(LEN1), -np.sin(phase) / math.sqrt(LEN1)
    straight = np.stack([re, im], 1).reshape(2 * LEN1, LEN1)
    swapped = np.stack([im, -re], 1).reshape(2 * LEN1, LEN1)
    return straight, swapped


def twist_tables():
    k1 = np.repeat(np.arange(LEN1), 2)
    b = np.arange(128) % B
    q = 2 * np.pi * k1[:, None] * b[None, :] / LENGTH
    p = 2 * np.pi * k1[None, :] * (B * np.arange(COL))[:, None] / LENGTH
    pt = np.zeros((COL, 8, 2 * LEN1))
    pt[:, 0] = np.cos(p)
    pt[:, 1] = np.sin(p)
    return np.cos(q), np.sin(q), pt


def second_table():
    k2 = np.arange(LEN2)[:, None]
    phase = 2 * np.pi * (k2 * np.arange(LEN2)[None, :] % LEN2) / LEN2
    cos, sin = np.cos(phase) / math.sqrt(LEN2), np.sin(phase) / math.sqrt(LEN2)
    real = np.stack([cos, sin], 2).reshape(LEN2, 2 * LEN2)
    imag = np.stack([-sin, cos], 2).reshape(LEN2, 2 * LEN2)
    return np.concatenate([real, imag], 0)


def order_table():
    table = np.zeros((ROW, 2, SEQS, SEQS, G))
    for r in range(ROW):
        for s in range(SEQS):
            table[r, 0, s, s, r] = 1
            table[r, 1, s, s, G - r if r else G // 2] = 1
    return table.reshape(4 * ROW, SEQS * G)


def front_kernel(x_ref, gain_ref, table_ref, w_hbm, y_ref, w_ref, rows_ref, send_ref, sems):
    width = F // IN_CHUNKS
    copies = []
    for i in range(IN_CHUNKS):
        cols = pl.ds(i * width, width)
        copies.append(pltpu.make_async_copy(w_hbm.at[:, cols], w_ref.at[:, cols], sems.at[i]))
        copies[-1].start()
    for a in range(A):
        for s in range(SEQS):
            rows_ref[pl.ds(8 * a + 4 * s, 4), :] = x_ref[s, a].astype(f32)
    x = rows_ref[...]
    mean_square = jnp.mean(x * x, axis=-1, keepdims=True)
    normed = (x * lax.rsqrt(mean_square + EPS) * gain_ref[...].astype(f32)).astype(bf16)
    parts = []
    for i in range(IN_CHUNKS):
        copies[i].wait()
        parts.append(jnp.dot(normed, w_ref[:, i * width : (i + 1) * width], preferred_element_type=f32))
    per = width // G
    table = table_ref[...]
    lane = lax.broadcasted_iota(jnp.int32, (ROW, 128), 1)
    first = (lane // 8) % 2 == 0
    for a in range(A):
        blocks = []
        for g in range(GROUPS):
            block = parts[g // per][8 * a : 8 * a + 8, (g % per) * G : (g % per + 1) * G]
            blocks += [block, block]
        stacked = jnp.concatenate(blocks, 0).astype(bf16)
        both = lax.dot_general(table, stacked, (((1,), (1,)), ((), ())), preferred_element_type=f32)
        send_ref[pl.ds(a, ROW, stride=A), :] = jnp.where(first, both[:ROW], both[ROW:]) * (1 / math.sqrt(G))
    y_ref[...] = send_ref[...].astype(bf16)


def swap_sublane_lane(x, sub, lane_step):
    row_bit = (lax.broadcasted_iota(jnp.int32, x.shape, 1) // sub) % 2
    lane_bit = (lax.broadcasted_iota(jnp.int32, x.shape, 2) // lane_step) % 2
    up = pltpu.roll(pltpu.roll(x, 8 - sub, 1), lane_step, 2)
    down = pltpu.roll(pltpu.roll(x, sub, 1), 128 - lane_step, 2)
    return jnp.where(row_bit == lane_bit, x, jnp.where(lane_bit == 1, up, down))


def first_kernel(z_ref, straight_ref, swapped_ref, qc_ref, qs_ref, pt_ref, o_ref):
    c = lax.axis_index("col")
    z = z_ref[...]
    p = pt_ref[c].T
    step = 128
    for i in range(2 * LEN1 // step):
        rows = slice(i * step, (i + 1) * step)
        u = jnp.dot(straight_ref[rows, :], z, preferred_element_type=f32)
        v = jnp.dot(swapped_ref[rows, :], z, preferred_element_type=f32)
        pc, ps = p[rows, 0:1], p[rows, 1:2]
        qc, qs = qc_ref[rows, :], qs_ref[rows, :]
        turned = u * (pc * qc - ps * qs) + v * (ps * qc + pc * qs)
        turned = turned.reshape(step // 8, 8, 128)
        turned = swap_sublane_lane(turned, 2, 1)
        turned = swap_sublane_lane(turned, 4, 2).astype(bf16)
        for j in range(step // 8):
            n = i * (step // 8) + j
            o_ref[n // 4, :, (n % 4) * 128 : (n % 4 + 1) * 128] = turned[j]


def second_kernel(v_ref, table_ref, s_ref, send_ref):
    head = lax.axis_index("row") == 0
    both = jnp.dot(table_ref[...], v_ref[...], preferred_element_type=f32)
    lane = lax.broadcasted_iota(jnp.int32, (LEN2, 128), 1)
    l_bit, s_bit = (lane // 8) % 2, (lane // 4) % 2
    real_here = jnp.logical_or(l_bit == 0, head)
    tiles = []
    for h in range(4):
        cols = slice(128 * h, 128 * (h + 1))
        tiles.append(jnp.where(real_here, both[:LEN2, cols], both[LEN2:, cols]))
    for shift, bit, pairs in ((8, l_bit, ((0, 2), (1, 3))), (4, s_bit, ((0, 1), (2, 3)))):
        for i, j in pairs:
            low, high = tiles[i], tiles[j]
            tiles[i] = jnp.where(bit == 0, low, pltpu.roll(high, shift, 1))
            tiles[j] = jnp.where(bit == 1, high, pltpu.roll(low, 128 - shift, 1))
    for s in range(SEQS):
        even, odd = tiles[s], tiles[2 + s]
        send_ref[pl.ds(s, LEN2, stride=4), :] = jnp.where(head, even, even + odd)
        send_ref[pl.ds(2 + s, LEN2, stride=4), :] = jnp.where(head, odd, even - odd)
    s_ref[...] = send_ref[...].astype(bf16)


def final_kernel(x_ref, order_ref, w_hbm, o_ref, w_ref, sems):
    width = D // OUT_CHUNKS
    copies = []
    for i in range(OUT_CHUNKS):
        cols = pl.ds(i * width, width)
        copies.append(pltpu.make_async_copy(w_hbm.at[:, cols], w_ref.at[:, cols], sems.at[i]))
        copies[-1].start()
    turned = x_ref[...].astype(f32).T.astype(bf16)
    placed = jnp.dot(turned, order_ref[...], preferred_element_type=f32)
    columns = []
    for g in range(GROUPS):
        rows = slice(16 * g, 16 * (g + 1))
        columns.append(jnp.concatenate([placed[rows, :G], placed[rows, G:]], 0))
    flat = jnp.concatenate(columns, 1).astype(bf16)
    for i in range(OUT_CHUNKS):
        copies[i].wait()
        cols = slice(i * width, (i + 1) * width)
        o_ref[:, cols] = jnp.dot(flat, w_ref[:, cols], preferred_element_type=f32).astype(bf16)


VMEM = pl.BlockSpec(memory_space=pltpu.VMEM)
ANY = pl.BlockSpec(memory_space=pl.ANY)


def body(tokens, norm_gain, w_mix_in, w_mix_out):
    def const(x, kind):
        return jnp.asarray(x.astype(kind))

    straight, swapped = first_tables()
    qc, qs, pt = twist_tables()
    y = pl.pallas_call(
        front_kernel,
        out_shape=jax.ShapeDtypeStruct((ROW * A, 128), bf16),
        in_specs=[VMEM, VMEM, VMEM, ANY],
        out_specs=VMEM,
        scratch_shapes=[
            pltpu.VMEM((D, F), bf16),
            pltpu.VMEM((32, D), f32),
            pltpu.VMEM((ROW * A, 128), f32),
            pltpu.SemaphoreType.DMA((IN_CHUNKS,)),
        ],
        name="front",
    )(tokens, norm_gain.reshape(1, D), const(channel_table(), bf16), w_mix_in)
    z = lax.all_to_all(y, "row", split_axis=0, concat_axis=0, tiled=True)
    o = pl.pallas_call(
        first_kernel,
        out_shape=jax.ShapeDtypeStruct((COL, 8, 512), bf16),
        in_specs=[VMEM] * 6,
        out_specs=VMEM,
        name="first",
    )(z, const(straight, bf16), const(swapped, bf16), const(qc, f32), const(qs, f32), const(pt, f32))
    v = lax.all_to_all(o, "col", split_axis=0, concat_axis=0, tiled=True)
    s = pl.pallas_call(
        second_kernel,
        out_shape=jax.ShapeDtypeStruct((4 * ROW, 128), bf16),
        in_specs=[VMEM] * 2,
        out_specs=VMEM,
        scratch_shapes=[pltpu.VMEM((4 * ROW, 128), f32)],
        name="second",
    )(v.reshape(2 * LEN2, 512), const(second_table(), bf16))
    x = lax.all_to_all(s, "row", split_axis=0, concat_axis=0, tiled=True)
    out = pl.pallas_call(
        final_kernel,
        out_shape=jax.ShapeDtypeStruct((SEQS * 16, D), bf16),
        in_specs=[VMEM, VMEM, ANY],
        out_specs=VMEM,
        scratch_shapes=[pltpu.VMEM((F, D), bf16), pltpu.SemaphoreType.DMA((OUT_CHUNKS,))],
        name="final",
    )(x, const(order_table(), bf16), w_mix_out)
    return out.reshape(SEQS, 1, 16, D)


def solution(mesh):
    placed = (P(None, "row", "col", None), P(), P(), P())
    return jax.shard_map(
        body, mesh=mesh, in_specs=placed, out_specs=P(None, "row", "col", None), check_vma=False
    )
```

```python
import math

import jax
import jax.numpy as jnp
import numpy as np
from jax import lax
from jax.experimental import pallas as pl
from jax.experimental.pallas import tpu as pltpu
from jax.sharding import PartitionSpec as P

D = 2048
F = 1024
G = 128
GROUPS = F // G
SEQS = 2
ROW = 64
COL = 16
A = 4
B = 4
LEN1 = ROW * A
LEN2 = COL * B
LENGTH = LEN1 * LEN2
EPS = 1e-06
IN_CHUNKS = 4
OUT_CHUNKS = 8
bf16 = jnp.bfloat16
f32 = jnp.float32


def channel_table():
    c = np.arange(G)[None, :]
    r = np.arange(ROW)[:, None]
    cos = np.cos(2 * np.pi * (c * r % G) / G)
    sin = np.sin(2 * np.pi * (c * r % G) / G)
    sin[0] = np.cos(np.pi * np.arange(G))
    return np.concatenate([cos, sin], 0)


def first_tables():
    k1 = np.arange(LEN1)[:, None]
    phase = 2 * np.pi * (k1 * np.arange(LEN1)[None, :] % LEN1) / LEN1
    re, im = np.cos(phase) / math.sqrt(LEN1), -np.sin(phase) / math.sqrt(LEN1)
    straight = np.stack([re, im], 1).reshape(2 * LEN1, LEN1)
    swapped = np.stack([im, -re], 1).reshape(2 * LEN1, LEN1)
    return straight, swapped


def twist(shape, col, start):
    row = lax.broadcasted_iota(jnp.int32, shape, 0) + start
    lane = lax.broadcasted_iota(jnp.int32, shape, 1)
    count = (row >> 1) * ((lane & (B - 1)) + B * col)
    quarter = LENGTH // 4
    quadrant = (count + quarter // 2) // quarter
    x = (count - quadrant * quarter).astype(f32) * (2 * math.pi / LENGTH)
    x2 = x * x
    sin = x * (1 + x2 * (-1 / 6 + x2 * (1 / 120 + x2 * (-1 / 5040 + x2 * (1 / 362880)))))
    cos = 1 + x2 * (-1 / 2 + x2 * (1 / 24 + x2 * (-1 / 720 + x2 * (1 / 40320))))
    odd = (quadrant & 1) == 1
    c, s = jnp.where(odd, sin, cos), jnp.where(odd, cos, sin)
    return jnp.where(((quadrant + 1) & 2) == 2, -c, c), jnp.where((quadrant & 2) == 2, -s, s)


def second_table():
    k2 = np.arange(LEN2)[:, None]
    phase = 2 * np.pi * (k2 * np.arange(LEN2)[None, :] % LEN2) / LEN2
    cos, sin = np.cos(phase) / math.sqrt(LEN2), np.sin(phase) / math.sqrt(LEN2)
    real = np.stack([cos, sin], 2).reshape(LEN2, 2 * LEN2)
    imag = np.stack([-sin, cos], 2).reshape(LEN2, 2 * LEN2)
    return np.concatenate([real, imag], 0)


def order_table():
    table = np.zeros((ROW, 2, SEQS, SEQS, G))
    for r in range(ROW):
        for s in range(SEQS):
            table[r, 0, s, s, r] = 1
            table[r, 1, s, s, G - r if r else G // 2] = 1
    return table.reshape(4 * ROW, SEQS * G)


def front_kernel(
    x_hbm, gain_hbm, table_hbm, w_hbm, straight_hbm, swapped_hbm,
    y_ref, cos_ref, sin_ref, straight_ref, swapped_ref,
    x_ref, gain_ref, table_ref, w_ref, rows_ref, send_ref, sems, w_sems,
):
    width = F // IN_CHUNKS
    x_copy = pltpu.make_async_copy(x_hbm, x_ref, sems.at[0])
    x_copy.start()
    gain_copy = pltpu.make_async_copy(gain_hbm, gain_ref, sems.at[4])
    gain_copy.start()
    copies = []
    for i in range(IN_CHUNKS):
        cols = pl.ds(i * width, width)
        copies.append(pltpu.make_async_copy(w_hbm.at[:, cols], w_ref.at[:, cols], w_sems.at[i]))
        copies[-1].start()
    table_copy = pltpu.make_async_copy(table_hbm, table_ref, sems.at[1])
    table_copy.start()
    others = [
        pltpu.make_async_copy(straight_hbm, straight_ref, sems.at[2]),
        pltpu.make_async_copy(swapped_hbm, swapped_ref, sems.at[3]),
    ]
    for copy in others:
        copy.start()
    col = lax.axis_index("col")
    for i in range(8):
        rows = slice(64 * i, 64 * (i + 1))
        cos_ref[rows, :], sin_ref[rows, :] = twist((64, 128), col, 64 * i)
    x_copy.wait()
    for a in range(A):
        for s in range(SEQS):
            rows_ref[pl.ds(8 * a + 4 * s, 4), :] = x_ref[s, a].astype(f32)
    x = rows_ref[...]
    mean_square = jnp.mean(x * x, axis=-1, keepdims=True)
    gain_copy.wait()
    gain = gain_ref[...].astype(f32).reshape(1, D)
    normed = (x * lax.rsqrt(mean_square + EPS) * gain).astype(bf16)
    parts = []
    for i in range(IN_CHUNKS):
        copies[i].wait()
        parts.append(jnp.dot(normed, w_ref[:, i * width : (i + 1) * width], preferred_element_type=f32))
    per = width // G
    table_copy.wait()
    table = table_ref[...]
    lane = lax.broadcasted_iota(jnp.int32, (ROW, 128), 1)
    first = (lane // 8) % 2 == 0
    for a in range(A):
        blocks = []
        for g in range(GROUPS):
            block = parts[g // per][8 * a : 8 * a + 8, (g % per) * G : (g % per + 1) * G]
            blocks += [block, block]
        stacked = jnp.concatenate(blocks, 0).astype(bf16)
        both = lax.dot_general(table, stacked, (((1,), (1,)), ((), ())), preferred_element_type=f32)
        send_ref[pl.ds(a, ROW, stride=A), :] = jnp.where(first, both[:ROW], both[ROW:]) * (1 / math.sqrt(G))
    y_ref[...] = send_ref[...].astype(bf16)
    for copy in others:
        copy.wait()


def swap_sublane_lane(x, sub, lane_step):
    row_bit = (lax.broadcasted_iota(jnp.int32, x.shape, 1) // sub) % 2
    lane_bit = (lax.broadcasted_iota(jnp.int32, x.shape, 2) // lane_step) % 2
    up = pltpu.roll(pltpu.roll(x, 8 - sub, 1), lane_step, 2)
    down = pltpu.roll(pltpu.roll(x, sub, 1), 128 - lane_step, 2)
    return jnp.where(row_bit == lane_bit, x, jnp.where(lane_bit == 1, up, down))


def first_kernel(z_ref, straight_ref, swapped_ref, cos_ref, sin_ref, o_ref):
    z = z_ref[...]
    step = 128
    for i in range(2 * LEN1 // step):
        rows = slice(i * step, (i + 1) * step)
        u = jnp.dot(straight_ref[rows, :], z, preferred_element_type=f32)
        v = jnp.dot(swapped_ref[rows, :], z, preferred_element_type=f32)
        turned = u * cos_ref[rows, :] + v * sin_ref[rows, :]
        turned = turned.reshape(step // 8, 8, 128)
        turned = swap_sublane_lane(turned, 2, 1)
        turned = swap_sublane_lane(turned, 4, 2).astype(bf16)
        for j in range(step // 8):
            n = i * (step // 8) + j
            o_ref[n // 4, :, (n % 4) * 128 : (n % 4 + 1) * 128] = turned[j]


def second_kernel(v_ref, table_ref, s_ref, send_ref):
    head = lax.axis_index("row") == 0
    both = jnp.dot(table_ref[...], v_ref[...], preferred_element_type=f32)
    lane = lax.broadcasted_iota(jnp.int32, (LEN2, 128), 1)
    l_bit, s_bit = (lane // 8) % 2, (lane // 4) % 2
    real_here = jnp.logical_or(l_bit == 0, head)
    tiles = []
    for h in range(4):
        cols = slice(128 * h, 128 * (h + 1))
        tiles.append(jnp.where(real_here, both[:LEN2, cols], both[LEN2:, cols]))
    for shift, bit, pairs in ((8, l_bit, ((0, 2), (1, 3))), (4, s_bit, ((0, 1), (2, 3)))):
        for i, j in pairs:
            low, high = tiles[i], tiles[j]
            tiles[i] = jnp.where(bit == 0, low, pltpu.roll(high, shift, 1))
            tiles[j] = jnp.where(bit == 1, high, pltpu.roll(low, 128 - shift, 1))
    for s in range(SEQS):
        even, odd = tiles[s], tiles[2 + s]
        send_ref[pl.ds(s, LEN2, stride=4), :] = jnp.where(head, even, even + odd)
        send_ref[pl.ds(2 + s, LEN2, stride=4), :] = jnp.where(head, odd, even - odd)
    s_ref[...] = send_ref[...].astype(bf16)


def final_kernel(x_ref, order_ref, w_ref, o_ref):
    width = D // OUT_CHUNKS
    turned = x_ref[...].astype(f32).T.astype(bf16)
    placed = jnp.dot(turned, order_ref[...], preferred_element_type=f32)
    columns = []
    for g in range(GROUPS):
        rows = slice(16 * g, 16 * (g + 1))
        columns.append(jnp.concatenate([placed[rows, :G], placed[rows, G:]], 0))
    flat = jnp.concatenate(columns, 1).astype(bf16)
    for i in range(OUT_CHUNKS):
        cols = slice(i * width, (i + 1) * width)
        o_ref[:, cols] = jnp.dot(flat, w_ref[:, cols], preferred_element_type=f32).astype(bf16)


VMEM = pl.BlockSpec(memory_space=pltpu.VMEM)
HBM = pl.BlockSpec(memory_space=pltpu.HBM)


def small(mib):
    return pltpu.CompilerParams(vmem_limit_bytes=mib << 20)


def in_hbm(x):
    return pltpu.with_memory_space_constraint(x, pltpu.HBM)


def shape(*dims, kind=bf16):
    return jax.ShapeDtypeStruct(dims, kind)


def body(tokens, norm_gain, w_mix_in, w_mix_out):
    def const(x):
        return jnp.asarray(x.astype(bf16))

    straight, swapped = first_tables()
    y, cos, sin, straight, swapped = pl.pallas_call(
        front_kernel,
        out_shape=[
            shape(ROW * A, 128),
            shape(2 * LEN1, 128, kind=f32),
            shape(2 * LEN1, 128, kind=f32),
            shape(2 * LEN1, LEN1),
            shape(2 * LEN1, LEN1),
        ],
        in_specs=[HBM] * 6,
        out_specs=[VMEM] * 5,
        scratch_shapes=[
            pltpu.VMEM((SEQS, A, B, D), bf16),
            pltpu.VMEM((D,), bf16),
            pltpu.VMEM((G, G), bf16),
            pltpu.VMEM((D, F), bf16),
            pltpu.VMEM((32, D), f32),
            pltpu.VMEM((ROW * A, 128), f32),
            pltpu.SemaphoreType.DMA((5,)),
            pltpu.SemaphoreType.DMA((IN_CHUNKS,)),
        ],
        compiler_params=small(16),
        name="front",
    )(
        in_hbm(tokens),
        in_hbm(norm_gain),
        in_hbm(const(channel_table())),
        in_hbm(w_mix_in),
        in_hbm(const(straight)),
        in_hbm(const(swapped)),
    )
    z = lax.all_to_all(y, "row", split_axis=0, concat_axis=0, tiled=True)
    o = pl.pallas_call(
        first_kernel,
        out_shape=shape(COL, 8, 512),
        in_specs=[VMEM] * 5,
        out_specs=VMEM,
        compiler_params=small(8),
        cost_estimate=pl.CostEstimate(flops=10**10, bytes_accessed=10**7, transcendentals=0),
        name="first",
    )(z, straight, swapped, cos, sin)
    v = lax.all_to_all(o, "col", split_axis=0, concat_axis=0, tiled=True)
    s = pl.pallas_call(
        second_kernel,
        out_shape=shape(4 * ROW, 128),
        in_specs=[VMEM] * 2,
        out_specs=VMEM,
        scratch_shapes=[pltpu.VMEM((4 * ROW, 128), f32)],
        compiler_params=small(8),
        cost_estimate=pl.CostEstimate(flops=10**10, bytes_accessed=10**7, transcendentals=0),
        name="second",
    )(v.reshape(2 * LEN2, 512), const(second_table()))
    x = lax.all_to_all(s, "row", split_axis=0, concat_axis=0, tiled=True)
    out = pl.pallas_call(
        final_kernel,
        out_shape=shape(SEQS * 16, D),
        in_specs=[VMEM] * 3,
        out_specs=VMEM,
        compiler_params=small(16),
        name="final",
    )(x, const(order_table()), w_mix_out)
    return out.reshape(SEQS, 1, 16, D)


def solution(mesh):
    placed = (P(None, "row", "col", None), P(), P(), P())
    return jax.shard_map(
        body, mesh=mesh, in_specs=placed, out_specs=P(None, "row", "col", None), check_vma=False
    )
```

```python
import math

import jax
import jax.numpy as jnp
import numpy as np
from jax import lax
from jax.experimental import pallas as pl
from jax.experimental.pallas import tpu as pltpu
from jax.sharding import PartitionSpec as P

D = 2048
F = 1024
G = 128
GROUPS = F // G
SEQS = 2
ROW = 64
COL = 16
A = 4
B = 4
LEN1 = ROW * A
LEN2 = COL * B
LENGTH = LEN1 * LEN2
EPS = 1e-06
IN_CHUNKS = 8
OUT_CHUNKS = 8
bf16 = jnp.bfloat16
f32 = jnp.float32


def channel_table():
    c = np.arange(G)[None, :]
    r = np.arange(ROW)[:, None]
    cos = np.cos(2 * np.pi * (c * r % G) / G)
    sin = np.sin(2 * np.pi * (c * r % G) / G)
    sin[0] = np.cos(np.pi * np.arange(G))
    return np.concatenate([cos, sin], 0)


def first_tables():
    k1 = np.arange(LEN1)[:, None]
    phase = 2 * np.pi * (k1 * np.arange(LEN1)[None, :] % LEN1) / LEN1
    re, im = np.cos(phase) / math.sqrt(LEN1), -np.sin(phase) / math.sqrt(LEN1)
    straight = np.stack([re, im], 1).reshape(2 * LEN1, LEN1)
    swapped = np.stack([im, -re], 1).reshape(2 * LEN1, LEN1)
    return straight, swapped


def twist(shape, col, start):
    row = lax.broadcasted_iota(jnp.int32, shape, 0) + start
    lane = lax.broadcasted_iota(jnp.int32, shape, 1)
    count = (row >> 1) * ((lane & (B - 1)) + B * col)
    quarter = LENGTH // 4
    quadrant = (count + quarter // 2) // quarter
    x = (count - quadrant * quarter).astype(f32) * (2 * math.pi / LENGTH)
    x2 = x * x
    sin = x * (1 + x2 * (-1 / 6 + x2 * (1 / 120 + x2 * (-1 / 5040 + x2 * (1 / 362880)))))
    cos = 1 + x2 * (-1 / 2 + x2 * (1 / 24 + x2 * (-1 / 720 + x2 * (1 / 40320))))
    odd = (quadrant & 1) == 1
    c, s = jnp.where(odd, sin, cos), jnp.where(odd, cos, sin)
    return jnp.where(((quadrant + 1) & 2) == 2, -c, c), jnp.where((quadrant & 2) == 2, -s, s)


def second_table():
    k2 = np.arange(LEN2)[:, None]
    phase = 2 * np.pi * (k2 * np.arange(LEN2)[None, :] % LEN2) / LEN2
    cos, sin = np.cos(phase) / math.sqrt(LEN2), np.sin(phase) / math.sqrt(LEN2)
    real = np.stack([cos, sin], 2).reshape(LEN2, 2 * LEN2)
    imag = np.stack([-sin, cos], 2).reshape(LEN2, 2 * LEN2)
    return np.concatenate([real, imag], 0)


def order_table():
    table = np.zeros((ROW, 2, SEQS, SEQS, G))
    for r in range(ROW):
        for s in range(SEQS):
            table[r, 0, s, s, r] = 1
            table[r, 1, s, s, G - r if r else G // 2] = 1
    return table.reshape(4 * ROW, SEQS * G)


def front_kernel(
    x_hbm, gain_hbm, table_hbm, w_hbm, straight_hbm, swapped_hbm,
    y_ref, cos_ref, sin_ref, straight_ref, swapped_ref,
    x_ref, gain_ref, table_ref, w_ref, rows_ref, send_ref, sems, w_sems,
):
    depth = D // IN_CHUNKS
    x_copy = pltpu.make_async_copy(x_hbm, x_ref, sems.at[0])
    x_copy.start()
    gain_copy = pltpu.make_async_copy(gain_hbm, gain_ref, sems.at[4])
    gain_copy.start()
    table_copy = pltpu.make_async_copy(table_hbm, table_ref, sems.at[1])
    table_copy.start()
    copies = []
    for i in range(IN_CHUNKS):
        part = pl.ds(i * depth, depth)
        copies.append(pltpu.make_async_copy(w_hbm.at[part], w_ref.at[part], w_sems.at[i]))
        copies[-1].start()
    others = [
        pltpu.make_async_copy(straight_hbm, straight_ref, sems.at[2]),
        pltpu.make_async_copy(swapped_hbm, swapped_ref, sems.at[3]),
    ]
    for copy in others:
        copy.start()
    col = lax.axis_index("col")
    for i in range(8):
        rows = slice(64 * i, 64 * (i + 1))
        cos_ref[rows, :], sin_ref[rows, :] = twist((64, 128), col, 64 * i)
    x_copy.wait()
    for a in range(A):
        for s in range(SEQS):
            rows_ref[pl.ds(8 * a + 4 * s, 4), :] = x_ref[s, a].astype(f32)
    x = rows_ref[...]
    mean_square = jnp.mean(x * x, axis=-1, keepdims=True)
    gain_copy.wait()
    gain = gain_ref[...].astype(f32).reshape(1, D)
    normed = (x * lax.rsqrt(mean_square + EPS) * gain).astype(bf16)
    mixed = jnp.zeros((32, F), f32)
    for i in range(IN_CHUNKS):
        copies[i].wait()
        part = slice(i * depth, (i + 1) * depth)
        mixed += jnp.dot(normed[:, part], w_ref[part, :], preferred_element_type=f32)
    table_copy.wait()
    table = table_ref[...]
    lane = lax.broadcasted_iota(jnp.int32, (ROW, 128), 1)
    first = (lane // 8) % 2 == 0
    for pair in range(A // 2):
        blocks = []
        for a in (2 * pair, 2 * pair + 1):
            for g in range(GROUPS):
                block = mixed[8 * a : 8 * a + 8, g * G : (g + 1) * G]
                blocks += [block, block]
        stacked = jnp.concatenate(blocks, 0).astype(bf16)
        both = lax.dot_general(table, stacked, (((1,), (1,)), ((), ())), preferred_element_type=f32)
        for i in range(2):
            lanes = slice(128 * i, 128 * (i + 1))
            picked = jnp.where(first, both[:ROW, lanes], both[ROW:, lanes]) * (1 / math.sqrt(G))
            send_ref[pl.ds(2 * pair + i, ROW, stride=A), :] = picked
    y_ref[...] = send_ref[...].astype(bf16)
    for copy in others:
        copy.wait()


def swap_sublane_lane(x, sub, lane_step):
    row_bit = (lax.broadcasted_iota(jnp.int32, x.shape, 1) // sub) % 2
    lane_bit = (lax.broadcasted_iota(jnp.int32, x.shape, 2) // lane_step) % 2
    up = pltpu.roll(pltpu.roll(x, 8 - sub, 1), lane_step, 2)
    down = pltpu.roll(pltpu.roll(x, sub, 1), 128 - lane_step, 2)
    return jnp.where(row_bit == lane_bit, x, jnp.where(lane_bit == 1, up, down))


def first_kernel(z_ref, straight_ref, swapped_ref, cos_ref, sin_ref, o_ref):
    z = z_ref[...]
    step = 128
    for i in range(2 * LEN1 // step):
        rows = slice(i * step, (i + 1) * step)
        u = jnp.dot(straight_ref[rows, :], z, preferred_element_type=f32)
        v = jnp.dot(swapped_ref[rows, :], z, preferred_element_type=f32)
        turned = u * cos_ref[rows, :] + v * sin_ref[rows, :]
        turned = turned.reshape(step // 8, 8, 128)
        turned = swap_sublane_lane(turned, 2, 1)
        turned = swap_sublane_lane(turned, 4, 2).astype(bf16)
        for j in range(step // 8):
            n = i * (step // 8) + j
            o_ref[n // 4, :, (n % 4) * 128 : (n % 4 + 1) * 128] = turned[j]


def second_kernel(v_ref, table_ref, s_ref, send_ref):
    head = lax.axis_index("row") == 0
    both = jnp.dot(table_ref[...], v_ref[...], preferred_element_type=f32)
    lane = lax.broadcasted_iota(jnp.int32, (LEN2, 128), 1)
    l_bit, s_bit = (lane // 8) % 2, (lane // 4) % 2
    real_here = jnp.logical_or(l_bit == 0, head)
    tiles = []
    for h in range(4):
        cols = slice(128 * h, 128 * (h + 1))
        tiles.append(jnp.where(real_here, both[:LEN2, cols], both[LEN2:, cols]))
    for shift, bit, pairs in ((8, l_bit, ((0, 2), (1, 3))), (4, s_bit, ((0, 1), (2, 3)))):
        for i, j in pairs:
            low, high = tiles[i], tiles[j]
            tiles[i] = jnp.where(bit == 0, low, pltpu.roll(high, shift, 1))
            tiles[j] = jnp.where(bit == 1, high, pltpu.roll(low, 128 - shift, 1))
    for s in range(SEQS):
        even, odd = tiles[s], tiles[2 + s]
        send_ref[pl.ds(s, LEN2, stride=4), :] = jnp.where(head, even, even + odd)
        send_ref[pl.ds(2 + s, LEN2, stride=4), :] = jnp.where(head, odd, even - odd)
    s_ref[...] = send_ref[...].astype(bf16)


def final_kernel(x_ref, order_ref, w_ref, o_ref):
    width = D // OUT_CHUNKS
    turned = x_ref[...].astype(f32).T.astype(bf16)
    placed = jnp.dot(turned, order_ref[...], preferred_element_type=f32)
    columns = []
    for g in range(GROUPS):
        rows = slice(16 * g, 16 * (g + 1))
        columns.append(jnp.concatenate([placed[rows, :G], placed[rows, G:]], 0))
    flat = jnp.concatenate(columns, 1).astype(bf16)
    for i in range(OUT_CHUNKS):
        cols = slice(i * width, (i + 1) * width)
        o_ref[:, cols] = jnp.dot(flat, w_ref[:, cols], preferred_element_type=f32).astype(bf16)


VMEM = pl.BlockSpec(memory_space=pltpu.VMEM)
HBM = pl.BlockSpec(memory_space=pltpu.HBM)


def small(mib):
    return pltpu.CompilerParams(vmem_limit_bytes=mib << 20)


def in_hbm(x):
    return pltpu.with_memory_space_constraint(x, pltpu.HBM)


def shape(*dims, kind=bf16):
    return jax.ShapeDtypeStruct(dims, kind)


def const(x):
    return jnp.asarray(x.astype(bf16))


def front(tokens, norm_gain, w_mix_in):
    straight, swapped = first_tables()
    return pl.pallas_call(
        front_kernel,
        out_shape=[
            shape(ROW * A, 128),
            shape(2 * LEN1, 128, kind=f32),
            shape(2 * LEN1, 128, kind=f32),
            shape(2 * LEN1, LEN1),
            shape(2 * LEN1, LEN1),
        ],
        in_specs=[HBM] * 6,
        out_specs=[VMEM] * 5,
        scratch_shapes=[
            pltpu.VMEM((SEQS, A, B, D), bf16),
            pltpu.VMEM((D,), bf16),
            pltpu.VMEM((G, G), bf16),
            pltpu.VMEM((D, F), bf16),
            pltpu.VMEM((32, D), f32),
            pltpu.VMEM((ROW * A, 128), f32),
            pltpu.SemaphoreType.DMA((5,)),
            pltpu.SemaphoreType.DMA((IN_CHUNKS,)),
        ],
        compiler_params=small(16),
        name="front",
    )(
        in_hbm(tokens),
        in_hbm(norm_gain),
        in_hbm(const(channel_table())),
        in_hbm(w_mix_in),
        in_hbm(const(straight)),
        in_hbm(const(swapped)),
    )


def first(z, straight, swapped, cos, sin):
    return pl.pallas_call(
        first_kernel,
        out_shape=shape(COL, 8, 512),
        in_specs=[VMEM] * 5,
        out_specs=VMEM,
        compiler_params=small(8),
        cost_estimate=pl.CostEstimate(flops=10**10, bytes_accessed=10**7, transcendentals=0),
        name="first",
    )(z, straight, swapped, cos, sin)


def second(v):
    return pl.pallas_call(
        second_kernel,
        out_shape=shape(4 * ROW, 128),
        in_specs=[VMEM] * 2,
        out_specs=VMEM,
        scratch_shapes=[pltpu.VMEM((4 * ROW, 128), f32)],
        compiler_params=small(8),
        cost_estimate=pl.CostEstimate(flops=10**10, bytes_accessed=10**7, transcendentals=0),
        name="second",
    )(v, const(second_table()))


def final(x, w_mix_out):
    return pl.pallas_call(
        final_kernel,
        out_shape=shape(SEQS * 16, D),
        in_specs=[VMEM] * 3,
        out_specs=VMEM,
        compiler_params=small(16),
        name="final",
    )(x, const(order_table()), w_mix_out)


def body(tokens, norm_gain, w_mix_in, w_mix_out):
    y, cos, sin, straight, swapped = front(tokens, norm_gain, w_mix_in)
    z = lax.all_to_all(y, "row", split_axis=0, concat_axis=0, tiled=True)
    o = first(z, straight, swapped, cos, sin)
    v = lax.all_to_all(o, "col", split_axis=0, concat_axis=0, tiled=True)
    s = second(v.reshape(2 * LEN2, 512))
    x = lax.all_to_all(s, "row", split_axis=0, concat_axis=0, tiled=True)
    return final(x, w_mix_out).reshape(SEQS, 1, 16, D)


def solution(mesh):
    placed = (P(None, "row", "col", None), P(), P(), P())
    return jax.shard_map(
        body, mesh=mesh, in_specs=placed, out_specs=P(None, "row", "col", None), check_vma=False
    )
```

```python
import math

import jax
import jax.numpy as jnp
import numpy as np
from jax import lax
from jax.experimental import pallas as pl
from jax.experimental.pallas import tpu as pltpu
from jax.sharding import PartitionSpec as P

D = 2048
F = 1024
G = 128
GROUPS = F // G
SEQS = 2
ROW = 64
COL = 16
A = 4
B = 4
LEN1 = ROW * A
LEN2 = COL * B
LENGTH = LEN1 * LEN2
EPS = 1e-06
IN_CHUNKS = 8
OUT_CHUNKS = 8
bf16 = jnp.bfloat16
f32 = jnp.float32


def channel_table():
    c = np.arange(G)[None, :]
    r = np.arange(ROW)[:, None]
    cos = np.cos(2 * np.pi * (c * r % G) / G)
    sin = np.sin(2 * np.pi * (c * r % G) / G)
    sin[0] = np.cos(np.pi * np.arange(G))
    return np.concatenate([cos, sin], 0)


def first_tables():
    k1 = np.arange(LEN1)[:, None]
    phase = 2 * np.pi * (k1 * np.arange(LEN1)[None, :] % LEN1) / LEN1
    re, im = np.cos(phase) / math.sqrt(LEN1), -np.sin(phase) / math.sqrt(LEN1)
    straight = np.stack([re, im], 1).reshape(2 * LEN1, LEN1)
    swapped = np.stack([im, -re], 1).reshape(2 * LEN1, LEN1)
    return straight, swapped


def twist(shape, col, start):
    row = lax.broadcasted_iota(jnp.int32, shape, 0) + start
    lane = lax.broadcasted_iota(jnp.int32, shape, 1)
    count = (row >> 1) * ((lane & (B - 1)) + B * col)
    quarter = LENGTH // 4
    quadrant = (count + quarter // 2) // quarter
    x = (count - quadrant * quarter).astype(f32) * (2 * math.pi / LENGTH)
    x2 = x * x
    sin = x * (1 + x2 * (-1 / 6 + x2 * (1 / 120 + x2 * (-1 / 5040 + x2 * (1 / 362880)))))
    cos = 1 + x2 * (-1 / 2 + x2 * (1 / 24 + x2 * (-1 / 720 + x2 * (1 / 40320))))
    odd = (quadrant & 1) == 1
    c, s = jnp.where(odd, sin, cos), jnp.where(odd, cos, sin)
    return jnp.where(((quadrant + 1) & 2) == 2, -c, c), jnp.where((quadrant & 2) == 2, -s, s)


def second_table():
    k2 = np.arange(LEN2)[:, None]
    phase = 2 * np.pi * (k2 * np.arange(LEN2)[None, :] % LEN2) / LEN2
    cos, sin = np.cos(phase) / math.sqrt(LEN2), np.sin(phase) / math.sqrt(LEN2)
    real = np.stack([cos, sin], 2).reshape(LEN2, 2 * LEN2)
    imag = np.stack([-sin, cos], 2).reshape(LEN2, 2 * LEN2)
    return np.concatenate([real, imag], 0)


def order_table():
    table = np.zeros((ROW, 2, SEQS, SEQS, G))
    for r in range(ROW):
        for s in range(SEQS):
            table[r, 0, s, s, r] = 1
            table[r, 1, s, s, G - r if r else G // 2] = 1
    return table.reshape(4 * ROW, SEQS * G)


def front_kernel(
    x_hbm, gain_hbm, table_hbm, w_hbm, straight_hbm, swapped_hbm,
    y_ref, cos_ref, sin_ref, straight_ref, swapped_ref,
    x_ref, gain_ref, table_ref, w_ref, rows_ref, send_ref, sems, w_sems,
):
    depth = D // IN_CHUNKS
    x_copy = pltpu.make_async_copy(x_hbm, x_ref, sems.at[0])
    x_copy.start()
    gain_copy = pltpu.make_async_copy(gain_hbm, gain_ref, sems.at[4])
    gain_copy.start()
    table_copy = pltpu.make_async_copy(table_hbm, table_ref, sems.at[1])
    table_copy.start()
    copies = []
    for i in range(IN_CHUNKS):
        part = pl.ds(i * depth, depth)
        copies.append(pltpu.make_async_copy(w_hbm.at[part], w_ref.at[part], w_sems.at[i]))
        copies[-1].start()
    others = [
        pltpu.make_async_copy(straight_hbm, straight_ref, sems.at[2]),
        pltpu.make_async_copy(swapped_hbm, swapped_ref, sems.at[3]),
    ]
    for copy in others:
        copy.start()
    col = lax.axis_index("col")
    for i in range(8):
        rows = slice(64 * i, 64 * (i + 1))
        cos_ref[rows, :], sin_ref[rows, :] = twist((64, 128), col, 64 * i)
    x_copy.wait()
    for a in range(A):
        for s in range(SEQS):
            rows_ref[pl.ds(8 * a + 4 * s, 4), :] = x_ref[s, a].astype(f32)
    x = rows_ref[...]
    mean_square = jnp.mean(x * x, axis=-1, keepdims=True)
    gain_copy.wait()
    gain = gain_ref[...].astype(f32).reshape(1, D)
    normed = (x * lax.rsqrt(mean_square + EPS) * gain).astype(bf16)
    mixed = jnp.zeros((32, F), f32)
    for i in range(IN_CHUNKS):
        copies[i].wait()
        part = slice(i * depth, (i + 1) * depth)
        mixed += jnp.dot(normed[:, part], w_ref[part, :], preferred_element_type=f32)
    table_copy.wait()
    table = table_ref[...]
    lane = lax.broadcasted_iota(jnp.int32, (ROW, 128), 1)
    first = (lane // 8) % 2 == 0
    for pair in range(A // 2):
        blocks = []
        for a in (2 * pair, 2 * pair + 1):
            for g in range(GROUPS):
                block = mixed[8 * a : 8 * a + 8, g * G : (g + 1) * G]
                blocks += [block, block]
        stacked = jnp.concatenate(blocks, 0).astype(bf16)
        both = lax.dot_general(table, stacked, (((1,), (1,)), ((), ())), preferred_element_type=f32)
        for i in range(2):
            lanes = slice(128 * i, 128 * (i + 1))
            picked = jnp.where(first, both[:ROW, lanes], both[ROW:, lanes]) * (1 / math.sqrt(G))
            send_ref[pl.ds(2 * pair + i, ROW, stride=A), :] = picked
    y_ref[...] = send_ref[...].astype(bf16)
    for copy in others:
        copy.wait()


def swap_sublane_lane(x, sub, lane_step):
    row_bit = (lax.broadcasted_iota(jnp.int32, x.shape, 1) // sub) % 2
    lane_bit = (lax.broadcasted_iota(jnp.int32, x.shape, 2) // lane_step) % 2
    up = pltpu.roll(pltpu.roll(x, 8 - sub, 1), lane_step, 2)
    down = pltpu.roll(pltpu.roll(x, sub, 1), 128 - lane_step, 2)
    return jnp.where(row_bit == lane_bit, x, jnp.where(lane_bit == 1, up, down))


def first_kernel(z_ref, straight_ref, swapped_ref, cos_ref, sin_ref, o_ref):
    z = z_ref[...]
    step = 128
    for i in range(2 * LEN1 // step):
        rows = slice(i * step, (i + 1) * step)
        u = jnp.dot(straight_ref[rows, :], z, preferred_element_type=f32)
        v = jnp.dot(swapped_ref[rows, :], z, preferred_element_type=f32)
        turned = u * cos_ref[rows, :] + v * sin_ref[rows, :]
        turned = turned.reshape(step // 8, 8, 128)
        turned = swap_sublane_lane(turned, 2, 1)
        turned = swap_sublane_lane(turned, 4, 2).astype(bf16)
        for j in range(step // 8):
            n = i * (step // 8) + j
            o_ref[n // 4, :, (n % 4) * 128 : (n % 4 + 1) * 128] = turned[j]


def second_kernel(v_ref, table_ref, s_ref, send_ref):
    head = lax.axis_index("row") == 0
    both = jnp.dot(table_ref[...], v_ref[...], preferred_element_type=f32)
    lane = lax.broadcasted_iota(jnp.int32, (LEN2, 128), 1)
    l_bit, s_bit = (lane // 8) % 2, (lane // 4) % 2
    real_here = jnp.logical_or(l_bit == 0, head)
    tiles = []
    for h in range(4):
        cols = slice(128 * h, 128 * (h + 1))
        tiles.append(jnp.where(real_here, both[:LEN2, cols], both[LEN2:, cols]))
    for shift, bit, pairs in ((8, l_bit, ((0, 2), (1, 3))), (4, s_bit, ((0, 1), (2, 3)))):
        for i, j in pairs:
            low, high = tiles[i], tiles[j]
            tiles[i] = jnp.where(bit == 0, low, pltpu.roll(high, shift, 1))
            tiles[j] = jnp.where(bit == 1, high, pltpu.roll(low, 128 - shift, 1))
    for s in range(SEQS):
        even, odd = tiles[s], tiles[2 + s]
        send_ref[pl.ds(s, LEN2, stride=4), :] = jnp.where(head, even, even + odd)
        send_ref[pl.ds(2 + s, LEN2, stride=4), :] = jnp.where(head, odd, even - odd)
    s_ref[...] = send_ref[...].astype(bf16)


def final_kernel(x_ref, order_ref, w_ref, o_ref):
    width = D // OUT_CHUNKS
    turned = x_ref[...].astype(f32).T.astype(bf16)
    placed = jnp.dot(turned, order_ref[...], preferred_element_type=f32)
    columns = []
    for g in range(GROUPS):
        rows = slice(16 * g, 16 * (g + 1))
        columns.append(jnp.concatenate([placed[rows, :G], placed[rows, G:]], 0))
    flat = jnp.concatenate(columns, 1).astype(bf16)
    for i in range(OUT_CHUNKS):
        cols = slice(i * width, (i + 1) * width)
        o_ref[:, cols] = jnp.dot(flat, w_ref[:, cols], preferred_element_type=f32).astype(bf16)


VMEM = pl.BlockSpec(memory_space=pltpu.VMEM)
HBM = pl.BlockSpec(memory_space=pltpu.HBM)


def small(mib):
    return pltpu.CompilerParams(vmem_limit_bytes=mib << 20)


def in_hbm(x):
    return pltpu.with_memory_space_constraint(x, pltpu.HBM)


def shape(*dims, kind=bf16):
    return jax.ShapeDtypeStruct(dims, kind)


def const(x):
    return jnp.asarray(x.astype(bf16))


def front(tokens, norm_gain, w_mix_in):
    straight, swapped = first_tables()
    return pl.pallas_call(
        front_kernel,
        out_shape=[
            shape(ROW * A, 128),
            shape(2 * LEN1, 128, kind=f32),
            shape(2 * LEN1, 128, kind=f32),
            shape(2 * LEN1, LEN1),
            shape(2 * LEN1, LEN1),
        ],
        in_specs=[HBM] * 6,
        out_specs=[VMEM] * 5,
        scratch_shapes=[
            pltpu.VMEM((SEQS, A, B, D), bf16),
            pltpu.VMEM((D,), bf16),
            pltpu.VMEM((G, G), bf16),
            pltpu.VMEM((D, F), bf16),
            pltpu.VMEM((32, D), f32),
            pltpu.VMEM((ROW * A, 128), f32),
            pltpu.SemaphoreType.DMA((5,)),
            pltpu.SemaphoreType.DMA((IN_CHUNKS,)),
        ],
        compiler_params=small(16),
        name="front",
    )(
        in_hbm(tokens),
        in_hbm(norm_gain),
        in_hbm(const(channel_table())),
        in_hbm(w_mix_in),
        in_hbm(const(straight)),
        in_hbm(const(swapped)),
    )


def first(z, straight, swapped, cos, sin):
    return pl.pallas_call(
        first_kernel,
        out_shape=shape(COL, 8, 512),
        in_specs=[VMEM] * 5,
        out_specs=VMEM,
        compiler_params=small(8),
        cost_estimate=pl.CostEstimate(flops=10**10, bytes_accessed=10**7, transcendentals=0),
        name="first",
    )(z, straight, swapped, cos, sin)


def second(v):
    return pl.pallas_call(
        second_kernel,
        out_shape=shape(4 * ROW, 128),
        in_specs=[VMEM] * 2,
        out_specs=VMEM,
        scratch_shapes=[pltpu.VMEM((4 * ROW, 128), f32)],
        compiler_params=small(8),
        cost_estimate=pl.CostEstimate(flops=10**4, bytes_accessed=10**4, transcendentals=0),
        name="second",
    )(v, const(second_table()))


def final(x, w_mix_out):
    return pl.pallas_call(
        final_kernel,
        out_shape=shape(SEQS * 16, D),
        in_specs=[VMEM] * 3,
        out_specs=VMEM,
        compiler_params=small(16),
        name="final",
    )(x, const(order_table()), w_mix_out)


def body(tokens, norm_gain, w_mix_in, w_mix_out):
    y, cos, sin, straight, swapped = front(tokens, norm_gain, w_mix_in)
    z = lax.all_to_all(y, "row", split_axis=0, concat_axis=0, tiled=True)
    o = first(z, straight, swapped, cos, sin)
    v = lax.all_to_all(o, "col", split_axis=0, concat_axis=0, tiled=True)
    s = second(v.reshape(2 * LEN2, 512))
    x = lax.all_to_all(s, "row", split_axis=0, concat_axis=0, tiled=True)
    return final(x, w_mix_out).reshape(SEQS, 1, 16, D)


def solution(mesh):
    placed = (P(None, "row", "col", None), P(), P(), P())
    return jax.shard_map(
        body, mesh=mesh, in_specs=placed, out_specs=P(None, "row", "col", None), check_vma=False
    )
```

```python
import math

import jax
import jax.numpy as jnp
import numpy as np
from jax import lax
from jax.experimental import pallas as pl
from jax.experimental.pallas import tpu as pltpu
from jax.sharding import PartitionSpec as P

D = 2048
F = 1024
G = 128
GROUPS = F // G
SEQS = 2
ROW = 64
COL = 16
A = 4
B = 4
LEN1 = ROW * A
LEN2 = COL * B
LENGTH = LEN1 * LEN2
EPS = 1e-06
IN_CHUNKS = 8
OUT_CHUNKS = 8
bf16 = jnp.bfloat16
f32 = jnp.float32


def channel_table():
    c = np.arange(G)[None, :]
    r = np.arange(ROW)[:, None]
    cos = np.cos(2 * np.pi * (c * r % G) / G)
    sin = np.sin(2 * np.pi * (c * r % G) / G)
    sin[0] = np.cos(np.pi * np.arange(G))
    return np.concatenate([cos, sin], 0)


def first_tables():
    k1 = np.arange(LEN1)[:, None]
    phase = 2 * np.pi * (k1 * np.arange(LEN1)[None, :] % LEN1) / LEN1
    re, im = np.cos(phase) / math.sqrt(LEN1), -np.sin(phase) / math.sqrt(LEN1)
    straight = np.stack([re, im], 1).reshape(2 * LEN1, LEN1)
    swapped = np.stack([im, -re], 1).reshape(2 * LEN1, LEN1)
    return straight, swapped


def twist(shape, col, start):
    row = lax.broadcasted_iota(jnp.int32, shape, 0) + start
    lane = lax.broadcasted_iota(jnp.int32, shape, 1)
    count = (row >> 1) * ((lane & (B - 1)) + B * col)
    quarter = LENGTH // 4
    quadrant = (count + quarter // 2) // quarter
    x = (count - quadrant * quarter).astype(f32) * (2 * math.pi / LENGTH)
    x2 = x * x
    sin = x * (1 + x2 * (-1 / 6 + x2 * (1 / 120 + x2 * (-1 / 5040 + x2 * (1 / 362880)))))
    cos = 1 + x2 * (-1 / 2 + x2 * (1 / 24 + x2 * (-1 / 720 + x2 * (1 / 40320))))
    odd = (quadrant & 1) == 1
    c, s = jnp.where(odd, sin, cos), jnp.where(odd, cos, sin)
    return jnp.where(((quadrant + 1) & 2) == 2, -c, c), jnp.where((quadrant & 2) == 2, -s, s)


def second_table():
    k2 = np.arange(LEN2)[:, None]
    phase = 2 * np.pi * (k2 * np.arange(LEN2)[None, :] % LEN2) / LEN2
    cos, sin = np.cos(phase) / math.sqrt(LEN2), np.sin(phase) / math.sqrt(LEN2)
    real = np.stack([cos, sin], 2).reshape(LEN2, 2 * LEN2)
    imag = np.stack([-sin, cos], 2).reshape(LEN2, 2 * LEN2)
    return np.concatenate([real, imag], 0)


def order_table():
    table = np.zeros((ROW, 2, SEQS, SEQS, G))
    for r in range(ROW):
        for s in range(SEQS):
            table[r, 0, s, s, r] = 1
            table[r, 1, s, s, G - r if r else G // 2] = 1
    return table.reshape(4 * ROW, SEQS * G)


def front_kernel(
    x_hbm, gain_hbm, table_hbm, w_hbm, straight_hbm, swapped_hbm,
    y_ref, cos_ref, sin_ref, straight_ref, swapped_ref,
    x_ref, gain_ref, table_ref, w_ref, rows_ref, send_ref, sems, w_sems,
):
    depth = D // IN_CHUNKS
    x_copy = pltpu.make_async_copy(x_hbm, x_ref, sems.at[0])
    x_copy.start()
    gain_copy = pltpu.make_async_copy(gain_hbm, gain_ref, sems.at[4])
    gain_copy.start()
    table_copy = pltpu.make_async_copy(table_hbm, table_ref, sems.at[1])
    table_copy.start()
    copies = []
    for i in range(IN_CHUNKS):
        part = pl.ds(i * depth, depth)
        copies.append(pltpu.make_async_copy(w_hbm.at[part], w_ref.at[part], w_sems.at[i]))
        copies[-1].start()
    others = [
        pltpu.make_async_copy(straight_hbm, straight_ref, sems.at[2]),
        pltpu.make_async_copy(swapped_hbm, swapped_ref, sems.at[3]),
    ]
    for copy in others:
        copy.start()
    col = lax.axis_index("col")
    for i in range(8):
        rows = slice(64 * i, 64 * (i + 1))
        cos_ref[rows, :], sin_ref[rows, :] = twist((64, 128), col, 64 * i)
    x_copy.wait()
    for a in range(A):
        for s in range(SEQS):
            rows_ref[pl.ds(8 * a + 4 * s, 4), :] = x_ref[s, a].astype(f32)
    x = rows_ref[...]
    gain_copy.wait()
    gain = gain_ref[...].astype(f32).reshape(1, D)
    gained = (x * gain).astype(bf16)
    scale = lax.rsqrt(jnp.mean(x * x, axis=-1, keepdims=True) + EPS)
    mixed = jnp.zeros((32, F), f32)
    for i in range(IN_CHUNKS):
        copies[i].wait()
        part = slice(i * depth, (i + 1) * depth)
        mixed += jnp.dot(gained[:, part], w_ref[part, :], preferred_element_type=f32)
    mixed = mixed * scale
    table_copy.wait()
    table = table_ref[...]
    lane = lax.broadcasted_iota(jnp.int32, (ROW, 128), 1)
    first = (lane // 8) % 2 == 0
    for pair in range(A // 2):
        blocks = []
        for a in (2 * pair, 2 * pair + 1):
            for g in range(GROUPS):
                block = mixed[8 * a : 8 * a + 8, g * G : (g + 1) * G]
                blocks += [block, block]
        stacked = jnp.concatenate(blocks, 0).astype(bf16)
        both = lax.dot_general(table, stacked, (((1,), (1,)), ((), ())), preferred_element_type=f32)
        for i in range(2):
            lanes = slice(128 * i, 128 * (i + 1))
            picked = jnp.where(first, both[:ROW, lanes], both[ROW:, lanes]) * (1 / math.sqrt(G))
            send_ref[pl.ds(2 * pair + i, ROW, stride=A), :] = picked
    y_ref[...] = send_ref[...].astype(bf16)
    for copy in others:
        copy.wait()


def swap_sublane_lane(x, sub, lane_step):
    row_bit = (lax.broadcasted_iota(jnp.int32, x.shape, 1) // sub) % 2
    lane_bit = (lax.broadcasted_iota(jnp.int32, x.shape, 2) // lane_step) % 2
    partner = jnp.where(lane_bit == 1, pltpu.roll(x, lane_step, 2), pltpu.roll(x, 128 - lane_step, 2))
    if sub == 4:
        partner = pltpu.roll(partner, 4, 1)
    else:
        partner = jnp.where(row_bit == 0, pltpu.roll(partner, 8 - sub, 1), pltpu.roll(partner, sub, 1))
    return jnp.where(row_bit == lane_bit, x, partner)


def first_kernel(z_ref, straight_ref, swapped_ref, cos_ref, sin_ref, o_ref):
    z = z_ref[...]
    step = 128
    for i in range(2 * LEN1 // step):
        rows = slice(i * step, (i + 1) * step)
        u = jnp.dot(straight_ref[rows, :], z, preferred_element_type=f32)
        v = jnp.dot(swapped_ref[rows, :], z, preferred_element_type=f32)
        turned = u * cos_ref[rows, :] + v * sin_ref[rows, :]
        turned = turned.reshape(step // 8, 8, 128)
        turned = swap_sublane_lane(turned, 2, 1)
        turned = swap_sublane_lane(turned, 4, 2).astype(bf16)
        for j in range(step // 8):
            n = i * (step // 8) + j
            o_ref[n // 4, :, (n % 4) * 128 : (n % 4 + 1) * 128] = turned[j]


def second_kernel(v_ref, table_ref, s_ref, send_ref):
    head = lax.axis_index("row") == 0
    both = jnp.dot(table_ref[...], v_ref[...], preferred_element_type=f32)
    lane = lax.broadcasted_iota(jnp.int32, (LEN2, 128), 1)
    l_bit, s_bit = (lane // 8) % 2, (lane // 4) % 2
    real_here = jnp.logical_or(l_bit == 0, head)
    tiles = []
    for h in range(4):
        cols = slice(128 * h, 128 * (h + 1))
        tiles.append(jnp.where(real_here, both[:LEN2, cols], both[LEN2:, cols]))
    for shift, bit, pairs in ((8, l_bit, ((0, 2), (1, 3))), (4, s_bit, ((0, 1), (2, 3)))):
        for i, j in pairs:
            low, high = tiles[i], tiles[j]
            tiles[i] = jnp.where(bit == 0, low, pltpu.roll(high, shift, 1))
            tiles[j] = jnp.where(bit == 1, high, pltpu.roll(low, 128 - shift, 1))
    for s in range(SEQS):
        even, odd = tiles[s], tiles[2 + s]
        send_ref[pl.ds(s, LEN2, stride=4), :] = jnp.where(head, even, even + odd)
        send_ref[pl.ds(2 + s, LEN2, stride=4), :] = jnp.where(head, odd, even - odd)
    s_ref[...] = send_ref[...].astype(bf16)


def final_kernel(x_ref, order_ref, w_ref, o_ref):
    width = D // OUT_CHUNKS
    turned = x_ref[...].astype(f32).T.astype(bf16)
    placed = jnp.dot(turned, order_ref[...], preferred_element_type=f32)
    columns = []
    for g in range(GROUPS):
        rows = slice(16 * g, 16 * (g + 1))
        columns.append(jnp.concatenate([placed[rows, :G], placed[rows, G:]], 0))
    flat = jnp.concatenate(columns, 1).astype(bf16)
    for i in range(OUT_CHUNKS):
        cols = slice(i * width, (i + 1) * width)
        o_ref[:, cols] = jnp.dot(flat, w_ref[:, cols], preferred_element_type=f32).astype(bf16)


VMEM = pl.BlockSpec(memory_space=pltpu.VMEM)
HBM = pl.BlockSpec(memory_space=pltpu.HBM)


def small(mib):
    return pltpu.CompilerParams(vmem_limit_bytes=mib << 20)


def in_hbm(x):
    return pltpu.with_memory_space_constraint(x, pltpu.HBM)


def shape(*dims, kind=bf16):
    return jax.ShapeDtypeStruct(dims, kind)


def const(x):
    return jnp.asarray(x.astype(bf16))


def front(tokens, norm_gain, w_mix_in):
    straight, swapped = first_tables()
    return pl.pallas_call(
        front_kernel,
        out_shape=[
            shape(ROW * A, 128),
            shape(2 * LEN1, 128, kind=f32),
            shape(2 * LEN1, 128, kind=f32),
            shape(2 * LEN1, LEN1),
            shape(2 * LEN1, LEN1),
        ],
        in_specs=[HBM] * 6,
        out_specs=[VMEM] * 5,
        scratch_shapes=[
            pltpu.VMEM((SEQS, A, B, D), bf16),
            pltpu.VMEM((D,), bf16),
            pltpu.VMEM((G, G), bf16),
            pltpu.VMEM((D, F), bf16),
            pltpu.VMEM((32, D), f32),
            pltpu.VMEM((ROW * A, 128), f32),
            pltpu.SemaphoreType.DMA((5,)),
            pltpu.SemaphoreType.DMA((IN_CHUNKS,)),
        ],
        compiler_params=small(16),
        name="front",
    )(
        in_hbm(tokens),
        in_hbm(norm_gain),
        in_hbm(const(channel_table())),
        in_hbm(w_mix_in),
        in_hbm(const(straight)),
        in_hbm(const(swapped)),
    )


def first(z, straight, swapped, cos, sin):
    return pl.pallas_call(
        first_kernel,
        out_shape=shape(COL, 8, 512),
        in_specs=[VMEM] * 5,
        out_specs=VMEM,
        compiler_params=small(8),
        cost_estimate=pl.CostEstimate(flops=10**10, bytes_accessed=10**7, transcendentals=0),
        name="first",
    )(z, straight, swapped, cos, sin)


def second(v):
    return pl.pallas_call(
        second_kernel,
        out_shape=shape(4 * ROW, 128),
        in_specs=[VMEM] * 2,
        out_specs=VMEM,
        scratch_shapes=[pltpu.VMEM((4 * ROW, 128), f32)],
        compiler_params=small(8),
        cost_estimate=pl.CostEstimate(flops=10**10, bytes_accessed=10**7, transcendentals=0),
        name="second",
    )(v, const(second_table()))


def final(x, w_mix_out):
    return pl.pallas_call(
        final_kernel,
        out_shape=shape(SEQS * 16, D),
        in_specs=[VMEM] * 3,
        out_specs=VMEM,
        compiler_params=small(16),
        name="final",
    )(x, const(order_table()), w_mix_out)


def body(tokens, norm_gain, w_mix_in, w_mix_out):
    y, cos, sin, straight, swapped = front(tokens, norm_gain, w_mix_in)
    z = lax.all_to_all(y, "row", split_axis=0, concat_axis=0, tiled=True)
    o = first(z, straight, swapped, cos, sin)
    v = lax.all_to_all(o, "col", split_axis=0, concat_axis=0, tiled=True)
    s = second(v.reshape(2 * LEN2, 512))
    x = lax.all_to_all(s, "row", split_axis=0, concat_axis=0, tiled=True)
    return final(x, w_mix_out).reshape(SEQS, 1, 16, D)


def solution(mesh):
    placed = (P(None, "row", "col", None), P(), P(), P())
    return jax.shard_map(
        body, mesh=mesh, in_specs=placed, out_specs=P(None, "row", "col", None), check_vma=False
    )
```

```python
import math

import jax
import jax.numpy as jnp
import numpy as np
from jax import lax
from jax.experimental import pallas as pl
from jax.experimental.pallas import tpu as pltpu
from jax.sharding import PartitionSpec as P

D = 2048
F = 1024
G = 128
GROUPS = F // G
SEQS = 2
ROW = 64
COL = 16
A = 4
B = 4
LEN1 = ROW * A
LEN2 = COL * B
LENGTH = LEN1 * LEN2
EPS = 1e-06
CHUNKS = ((0, 512), (512, 512), (1024, 256), (1280, 256), (1536, 256), (1792, 256))
IN_CHUNKS = len(CHUNKS)
OUT_CHUNKS = 8
bf16 = jnp.bfloat16
f32 = jnp.float32


def channel_table():
    c = np.arange(G)[None, :]
    r = np.arange(ROW)[:, None]
    cos = np.cos(2 * np.pi * (c * r % G) / G)
    sin = np.sin(2 * np.pi * (c * r % G) / G)
    sin[0] = np.cos(np.pi * np.arange(G))
    return np.concatenate([cos, sin], 0)


def first_tables():
    k1 = np.arange(LEN1)[:, None]
    phase = 2 * np.pi * (k1 * np.arange(LEN1)[None, :] % LEN1) / LEN1
    re, im = np.cos(phase) / math.sqrt(LEN1), -np.sin(phase) / math.sqrt(LEN1)
    straight = np.stack([re, im], 1).reshape(2 * LEN1, LEN1)
    swapped = np.stack([im, -re], 1).reshape(2 * LEN1, LEN1)
    return straight, swapped


def twist(shape, col, start):
    row = lax.broadcasted_iota(jnp.int32, shape, 0) + start
    lane = lax.broadcasted_iota(jnp.int32, shape, 1)
    count = (row >> 1) * ((lane & (B - 1)) + B * col)
    quarter = LENGTH // 4
    quadrant = (count + quarter // 2) // quarter
    x = (count - quadrant * quarter).astype(f32) * (2 * math.pi / LENGTH)
    x2 = x * x
    sin = x * (1 + x2 * (-1 / 6 + x2 * (1 / 120 + x2 * (-1 / 5040 + x2 * (1 / 362880)))))
    cos = 1 + x2 * (-1 / 2 + x2 * (1 / 24 + x2 * (-1 / 720 + x2 * (1 / 40320))))
    odd = (quadrant & 1) == 1
    c, s = jnp.where(odd, sin, cos), jnp.where(odd, cos, sin)
    return jnp.where(((quadrant + 1) & 2) == 2, -c, c), jnp.where((quadrant & 2) == 2, -s, s)


def second_table():
    k2 = np.arange(LEN2)[:, None]
    phase = 2 * np.pi * (k2 * np.arange(LEN2)[None, :] % LEN2) / LEN2
    cos, sin = np.cos(phase) / math.sqrt(LEN2), np.sin(phase) / math.sqrt(LEN2)
    real = np.stack([cos, sin], 2).reshape(LEN2, 2 * LEN2)
    imag = np.stack([-sin, cos], 2).reshape(LEN2, 2 * LEN2)
    return np.concatenate([real, imag], 0)


def order_table():
    table = np.zeros((ROW, 2, SEQS, SEQS, G))
    for r in range(ROW):
        for s in range(SEQS):
            table[r, 0, s, s, r] = 1
            table[r, 1, s, s, G - r if r else G // 2] = 1
    return table.reshape(4 * ROW, SEQS * G)


def front_kernel(
    x_hbm, gain_hbm, table_hbm, w_hbm, straight_hbm, swapped_hbm,
    y_ref, cos_ref, sin_ref, straight_ref, swapped_ref,
    x_ref, gain_ref, table_ref, w_ref, rows_ref, send_ref, sems, w_sems,
):
    x_copy = pltpu.make_async_copy(x_hbm, x_ref, sems.at[0])
    x_copy.start()
    gain_copy = pltpu.make_async_copy(gain_hbm, gain_ref, sems.at[4])
    gain_copy.start()
    table_copy = pltpu.make_async_copy(table_hbm, table_ref, sems.at[1])
    table_copy.start()
    copies = []
    for i in range(IN_CHUNKS):
        part = pl.ds(*CHUNKS[i])
        copies.append(pltpu.make_async_copy(w_hbm.at[part], w_ref.at[part], w_sems.at[i]))
        copies[-1].start()
    others = [
        pltpu.make_async_copy(straight_hbm, straight_ref, sems.at[2]),
        pltpu.make_async_copy(swapped_hbm, swapped_ref, sems.at[3]),
    ]
    for copy in others:
        copy.start()
    col = lax.axis_index("col")
    for i in range(8):
        rows = slice(64 * i, 64 * (i + 1))
        cos_ref[rows, :], sin_ref[rows, :] = twist((64, 128), col, 64 * i)
    x_copy.wait()
    for a in range(A):
        for s in range(SEQS):
            rows_ref[pl.ds(8 * a + 4 * s, 4), :] = x_ref[s, a].astype(f32)
    x = rows_ref[...]
    mean_square = jnp.mean(x * x, axis=-1, keepdims=True)
    gain_copy.wait()
    gain = gain_ref[...].astype(f32).reshape(1, D)
    normed = (x * lax.rsqrt(mean_square + EPS) * gain).astype(bf16)
    mixed = jnp.zeros((32, F), f32)
    for i in range(IN_CHUNKS):
        copies[i].wait()
        part = slice(CHUNKS[i][0], sum(CHUNKS[i]))
        mixed += jnp.dot(normed[:, part], w_ref[part, :], preferred_element_type=f32)
    table_copy.wait()
    table = table_ref[...]
    lane = lax.broadcasted_iota(jnp.int32, (ROW, 128), 1)
    first = (lane // 8) % 2 == 0
    for pair in range(A // 2):
        blocks = []
        for a in (2 * pair, 2 * pair + 1):
            for g in range(GROUPS):
                block = mixed[8 * a : 8 * a + 8, g * G : (g + 1) * G]
                blocks += [block, block]
        stacked = jnp.concatenate(blocks, 0).astype(bf16)
        both = lax.dot_general(table, stacked, (((1,), (1,)), ((), ())), preferred_element_type=f32)
        for i in range(2):
            lanes = slice(128 * i, 128 * (i + 1))
            picked = jnp.where(first, both[:ROW, lanes], both[ROW:, lanes]) * (1 / math.sqrt(G))
            send_ref[pl.ds(2 * pair + i, ROW, stride=A), :] = picked
    y_ref[...] = send_ref[...].astype(bf16)
    for copy in others:
        copy.wait()


def swap_sublane_lane(x, sub, lane_step):
    row_bit = (lax.broadcasted_iota(jnp.int32, x.shape, 1) // sub) % 2
    lane_bit = (lax.broadcasted_iota(jnp.int32, x.shape, 2) // lane_step) % 2
    up = pltpu.roll(pltpu.roll(x, 8 - sub, 1), lane_step, 2)
    down = pltpu.roll(pltpu.roll(x, sub, 1), 128 - lane_step, 2)
    return jnp.where(row_bit == lane_bit, x, jnp.where(lane_bit == 1, up, down))


def first_kernel(z_ref, straight_ref, swapped_ref, cos_ref, sin_ref, o_ref):
    z = z_ref[...]
    step = 128
    for i in range(2 * LEN1 // step):
        rows = slice(i * step, (i + 1) * step)
        u = jnp.dot(straight_ref[rows, :], z, preferred_element_type=f32)
        v = jnp.dot(swapped_ref[rows, :], z, preferred_element_type=f32)
        turned = u * cos_ref[rows, :] + v * sin_ref[rows, :]
        turned = turned.reshape(step // 8, 8, 128)
        turned = swap_sublane_lane(turned, 2, 1)
        turned = swap_sublane_lane(turned, 4, 2).astype(bf16)
        for j in range(step // 8):
            n = i * (step // 8) + j
            o_ref[n // 4, :, (n % 4) * 128 : (n % 4 + 1) * 128] = turned[j]


def second_kernel(v_ref, table_ref, s_ref, send_ref):
    head = lax.axis_index("row") == 0
    both = jnp.dot(table_ref[...], v_ref[...], preferred_element_type=f32)
    lane = lax.broadcasted_iota(jnp.int32, (LEN2, 128), 1)
    l_bit, s_bit = (lane // 8) % 2, (lane // 4) % 2
    real_here = jnp.logical_or(l_bit == 0, head)
    tiles = []
    for h in range(4):
        cols = slice(128 * h, 128 * (h + 1))
        tiles.append(jnp.where(real_here, both[:LEN2, cols], both[LEN2:, cols]))
    for shift, bit, pairs in ((8, l_bit, ((0, 2), (1, 3))), (4, s_bit, ((0, 1), (2, 3)))):
        for i, j in pairs:
            low, high = tiles[i], tiles[j]
            tiles[i] = jnp.where(bit == 0, low, pltpu.roll(high, shift, 1))
            tiles[j] = jnp.where(bit == 1, high, pltpu.roll(low, 128 - shift, 1))
    for s in range(SEQS):
        even, odd = tiles[s], tiles[2 + s]
        send_ref[pl.ds(s, LEN2, stride=4), :] = jnp.where(head, even, even + odd)
        send_ref[pl.ds(2 + s, LEN2, stride=4), :] = jnp.where(head, odd, even - odd)
    s_ref[...] = send_ref[...].astype(bf16)


def final_kernel(x_ref, order_ref, w_ref, o_ref):
    width = D // OUT_CHUNKS
    turned = x_ref[...].astype(f32).T.astype(bf16)
    placed = jnp.dot(turned, order_ref[...], preferred_element_type=f32)
    columns = []
    for g in range(GROUPS):
        rows = slice(16 * g, 16 * (g + 1))
        columns.append(jnp.concatenate([placed[rows, :G], placed[rows, G:]], 0))
    flat = jnp.concatenate(columns, 1).astype(bf16)
    for i in range(OUT_CHUNKS):
        cols = slice(i * width, (i + 1) * width)
        o_ref[:, cols] = jnp.dot(flat, w_ref[:, cols], preferred_element_type=f32).astype(bf16)


VMEM = pl.BlockSpec(memory_space=pltpu.VMEM)
HBM = pl.BlockSpec(memory_space=pltpu.HBM)


def small(mib):
    return pltpu.CompilerParams(vmem_limit_bytes=mib << 20)


def in_hbm(x):
    return pltpu.with_memory_space_constraint(x, pltpu.HBM)


def shape(*dims, kind=bf16):
    return jax.ShapeDtypeStruct(dims, kind)


def const(x):
    return jnp.asarray(x.astype(bf16))


def front(tokens, norm_gain, w_mix_in):
    straight, swapped = first_tables()
    return pl.pallas_call(
        front_kernel,
        out_shape=[
            shape(ROW * A, 128),
            shape(2 * LEN1, 128, kind=f32),
            shape(2 * LEN1, 128, kind=f32),
            shape(2 * LEN1, LEN1),
            shape(2 * LEN1, LEN1),
        ],
        in_specs=[HBM] * 6,
        out_specs=[VMEM] * 5,
        scratch_shapes=[
            pltpu.VMEM((SEQS, A, B, D), bf16),
            pltpu.VMEM((D,), bf16),
            pltpu.VMEM((G, G), bf16),
            pltpu.VMEM((D, F), bf16),
            pltpu.VMEM((32, D), f32),
            pltpu.VMEM((ROW * A, 128), f32),
            pltpu.SemaphoreType.DMA((5,)),
            pltpu.SemaphoreType.DMA((IN_CHUNKS,)),
        ],
        compiler_params=small(16),
        name="front",
    )(
        in_hbm(tokens),
        in_hbm(norm_gain),
        in_hbm(const(channel_table())),
        in_hbm(w_mix_in),
        in_hbm(const(straight)),
        in_hbm(const(swapped)),
    )


def first(z, straight, swapped, cos, sin):
    return pl.pallas_call(
        first_kernel,
        out_shape=shape(COL, 8, 512),
        in_specs=[VMEM] * 5,
        out_specs=VMEM,
        compiler_params=small(8),
        cost_estimate=pl.CostEstimate(flops=10**10, bytes_accessed=10**7, transcendentals=0),
        name="first",
    )(z, straight, swapped, cos, sin)


def second(v):
    return pl.pallas_call(
        second_kernel,
        out_shape=shape(4 * ROW, 128),
        in_specs=[VMEM] * 2,
        out_specs=VMEM,
        scratch_shapes=[pltpu.VMEM((4 * ROW, 128), f32)],
        compiler_params=small(8),
        cost_estimate=pl.CostEstimate(flops=10**10, bytes_accessed=10**7, transcendentals=0),
        name="second",
    )(v, const(second_table()))


def final(x, w_mix_out):
    return pl.pallas_call(
        final_kernel,
        out_shape=shape(SEQS * 16, D),
        in_specs=[VMEM] * 3,
        out_specs=VMEM,
        compiler_params=small(16),
        name="final",
    )(x, const(order_table()), w_mix_out)


def body(tokens, norm_gain, w_mix_in, w_mix_out):
    y, cos, sin, straight, swapped = front(tokens, norm_gain, w_mix_in)
    z = lax.all_to_all(y, "row", split_axis=0, concat_axis=0, tiled=True)
    o = first(z, straight, swapped, cos, sin)
    v = lax.all_to_all(o, "col", split_axis=0, concat_axis=0, tiled=True)
    s = second(v.reshape(2 * LEN2, 512))
    x = lax.all_to_all(s, "row", split_axis=0, concat_axis=0, tiled=True)
    return final(x, w_mix_out).reshape(SEQS, 1, 16, D)


def solution(mesh):
    placed = (P(None, "row", "col", None), P(), P(), P())
    return jax.shard_map(
        body, mesh=mesh, in_specs=placed, out_specs=P(None, "row", "col", None), check_vma=False
    )
```

```python
import math

import jax
import jax.numpy as jnp
import numpy as np
from jax import lax
from jax.experimental import pallas as pl
from jax.experimental.pallas import tpu as pltpu
from jax.sharding import PartitionSpec as P

D = 2048
F = 1024
G = 128
GROUPS = F // G
SEQS = 2
ROW = 64
COL = 16
A = 4
B = 4
LEN1 = ROW * A
LEN2 = COL * B
LENGTH = LEN1 * LEN2
EPS = 1e-06
IN_CHUNKS = 8
OUT_CHUNKS = 8
bf16 = jnp.bfloat16
f32 = jnp.float32


def channel_table():
    c = np.arange(G)[None, :]
    r = np.arange(ROW)[:, None]
    cos = np.cos(2 * np.pi * (c * r % G) / G)
    sin = np.sin(2 * np.pi * (c * r % G) / G)
    sin[0] = np.cos(np.pi * np.arange(G))
    return np.concatenate([cos, sin], 0)


def first_tables():
    k1 = np.arange(LEN1)[:, None]
    phase = 2 * np.pi * (k1 * np.arange(LEN1)[None, :] % LEN1) / LEN1
    re, im = np.cos(phase) / math.sqrt(LEN1), -np.sin(phase) / math.sqrt(LEN1)
    straight = np.stack([re, im], 1).reshape(2 * LEN1, LEN1)
    swapped = np.stack([im, -re], 1).reshape(2 * LEN1, LEN1)
    return straight, swapped


def twist(shape, col, start):
    row = lax.broadcasted_iota(jnp.int32, shape, 0) + start
    lane = lax.broadcasted_iota(jnp.int32, shape, 1)
    count = (row >> 1) * ((lane & (B - 1)) + B * col)
    quarter = LENGTH // 4
    quadrant = (count + quarter // 2) // quarter
    x = (count - quadrant * quarter).astype(f32) * (2 * math.pi / LENGTH)
    x2 = x * x
    sin = x * (1 + x2 * (-1 / 6 + x2 * (1 / 120 + x2 * (-1 / 5040 + x2 * (1 / 362880)))))
    cos = 1 + x2 * (-1 / 2 + x2 * (1 / 24 + x2 * (-1 / 720 + x2 * (1 / 40320))))
    odd = (quadrant & 1) == 1
    c, s = jnp.where(odd, sin, cos), jnp.where(odd, cos, sin)
    return jnp.where(((quadrant + 1) & 2) == 2, -c, c), jnp.where((quadrant & 2) == 2, -s, s)


def second_table():
    k2 = np.arange(LEN2)[:, None]
    phase = 2 * np.pi * (k2 * np.arange(LEN2)[None, :] % LEN2) / LEN2
    cos, sin = np.cos(phase) / math.sqrt(LEN2), np.sin(phase) / math.sqrt(LEN2)
    real = np.stack([cos, sin], 2).reshape(LEN2, 2 * LEN2)
    imag = np.stack([-sin, cos], 2).reshape(LEN2, 2 * LEN2)
    return np.concatenate([real, imag], 0)


def order_table():
    table = np.zeros((ROW, 2, SEQS, SEQS, G))
    for r in range(ROW):
        for s in range(SEQS):
            table[r, 0, s, s, r] = 1
            table[r, 1, s, s, G - r if r else G // 2] = 1
    return table.reshape(4 * ROW, SEQS * G)


def front_kernel(
    x_hbm, gain_hbm, table_hbm, w_hbm, straight_hbm, swapped_hbm,
    y_ref, cos_ref, sin_ref, straight_ref, swapped_ref,
    x_ref, gain_ref, table_ref, w_ref, rows_ref, send_ref, sems, w_sems,
):
    depth = D // IN_CHUNKS
    x_copy = pltpu.make_async_copy(x_hbm, x_ref, sems.at[0])
    x_copy.start()
    gain_copy = pltpu.make_async_copy(gain_hbm, gain_ref, sems.at[4])
    gain_copy.start()
    table_copy = pltpu.make_async_copy(table_hbm, table_ref, sems.at[1])
    table_copy.start()
    copies = []
    for i in range(IN_CHUNKS):
        part = pl.ds(i * depth, depth)
        copies.append(pltpu.make_async_copy(w_hbm.at[part], w_ref.at[part], w_sems.at[i]))
        copies[-1].start()
    others = [
        pltpu.make_async_copy(straight_hbm, straight_ref, sems.at[2]),
        pltpu.make_async_copy(swapped_hbm, swapped_ref, sems.at[3]),
    ]
    for copy in others:
        copy.start()
    col = lax.axis_index("col")
    for i in range(8):
        rows = slice(64 * i, 64 * (i + 1))
        cos_ref[rows, :], sin_ref[rows, :] = twist((64, 128), col, 64 * i)
    x_copy.wait()
    for a in range(A):
        for s in range(SEQS):
            rows_ref[pl.ds(8 * a + 4 * s, 4), :] = x_ref[s, a].astype(f32)
    x = rows_ref[...]
    mean_square = jnp.mean(x * x, axis=-1, keepdims=True)
    gain_copy.wait()
    gain = gain_ref[...].astype(f32).reshape(1, D)
    normed = (x * lax.rsqrt(mean_square + EPS) * gain).astype(bf16)
    mixed = jnp.zeros((32, F), f32)
    for i in range(IN_CHUNKS):
        copies[i].wait()
        part = slice(i * depth, (i + 1) * depth)
        mixed += jnp.dot(normed[:, part], w_ref[part, :], preferred_element_type=f32)
    table_copy.wait()
    table = table_ref[...]
    lane = lax.broadcasted_iota(jnp.int32, (ROW, 128), 1)
    first = (lane // 8) % 2 == 0
    for pair in range(A // 2):
        blocks = []
        for a in (2 * pair, 2 * pair + 1):
            for g in range(GROUPS):
                block = mixed[8 * a : 8 * a + 8, g * G : (g + 1) * G]
                blocks += [block, block]
        stacked = jnp.concatenate(blocks, 0).astype(bf16)
        both = lax.dot_general(table, stacked, (((1,), (1,)), ((), ())), preferred_element_type=f32)
        for i in range(2):
            lanes = slice(128 * i, 128 * (i + 1))
            picked = jnp.where(first, both[:ROW, lanes], both[ROW:, lanes]) * (1 / math.sqrt(G))
            send_ref[pl.ds(2 * pair + i, ROW, stride=A), :] = picked
    y_ref[...] = send_ref[...].astype(bf16)
    for copy in others:
        copy.wait()


def swap_sublane_lane(x, sub, lane_step):
    row_bit = (lax.broadcasted_iota(jnp.int32, x.shape, 1) // sub) % 2
    lane_bit = (lax.broadcasted_iota(jnp.int32, x.shape, 2) // lane_step) % 2
    up = pltpu.roll(pltpu.roll(x, 8 - sub, 1), lane_step, 2)
    down = pltpu.roll(pltpu.roll(x, sub, 1), 128 - lane_step, 2)
    return jnp.where(row_bit == lane_bit, x, jnp.where(lane_bit == 1, up, down))


def first_kernel(z_ref, straight_ref, swapped_ref, cos_ref, sin_ref, o_ref):
    z = z_ref[...]
    step = 128
    for i in range(2 * LEN1 // step):
        rows = slice(i * step, (i + 1) * step)
        u = jnp.dot(straight_ref[rows, :], z, preferred_element_type=f32)
        v = jnp.dot(swapped_ref[rows, :], z, preferred_element_type=f32)
        turned = u * cos_ref[rows, :] + v * sin_ref[rows, :]
        turned = turned.reshape(step // 8, 8, 128)
        turned = swap_sublane_lane(turned, 2, 1)
        turned = swap_sublane_lane(turned, 4, 2).astype(bf16)
        for j in range(step // 8):
            n = i * (step // 8) + j
            o_ref[n // 4, :, (n % 4) * 128 : (n % 4 + 1) * 128] = turned[j]


def second_kernel(v_ref, table_ref, s_ref, send_ref):
    head = lax.axis_index("row") == 0
    both = jnp.dot(table_ref[...], v_ref[...], preferred_element_type=f32)
    lane = lax.broadcasted_iota(jnp.int32, (LEN2, 128), 1)
    l_bit, s_bit = (lane // 8) % 2, (lane // 4) % 2
    real_here = jnp.logical_or(l_bit == 0, head)
    tiles = []
    for h in range(4):
        cols = slice(128 * h, 128 * (h + 1))
        tiles.append(jnp.where(real_here, both[:LEN2, cols], both[LEN2:, cols]))
    for shift, bit, pairs in ((8, l_bit, ((0, 2), (1, 3))), (4, s_bit, ((0, 1), (2, 3)))):
        for i, j in pairs:
            low, high = tiles[i], tiles[j]
            tiles[i] = jnp.where(bit == 0, low, pltpu.roll(high, shift, 1))
            tiles[j] = jnp.where(bit == 1, high, pltpu.roll(low, 128 - shift, 1))
    for s in range(SEQS):
        even, odd = tiles[s], tiles[2 + s]
        send_ref[pl.ds(s, LEN2, stride=4), :] = jnp.where(head, even, even + odd)
        send_ref[pl.ds(2 + s, LEN2, stride=4), :] = jnp.where(head, odd, even - odd)
    s_ref[...] = send_ref[...].astype(bf16)


def final_kernel(x_ref, order_ref, w_ref, o_ref):
    width = D // OUT_CHUNKS
    turned = x_ref[...].astype(f32).T.astype(bf16)
    placed = jnp.dot(turned, order_ref[...], preferred_element_type=f32)
    columns = []
    for g in range(GROUPS):
        rows = slice(16 * g, 16 * (g + 1))
        columns.append(jnp.concatenate([placed[rows, :G], placed[rows, G:]], 0))
    flat = jnp.concatenate(columns, 1).astype(bf16)
    for i in range(OUT_CHUNKS):
        cols = slice(i * width, (i + 1) * width)
        o_ref[:, cols] = jnp.dot(flat, w_ref[:, cols], preferred_element_type=f32).astype(bf16)


VMEM = pl.BlockSpec(memory_space=pltpu.VMEM)
HBM = pl.BlockSpec(memory_space=pltpu.HBM)


def small(mib):
    return pltpu.CompilerParams(vmem_limit_bytes=mib << 20)


def in_hbm(x):
    return pltpu.with_memory_space_constraint(x, pltpu.HBM)


def shape(*dims, kind=bf16):
    return jax.ShapeDtypeStruct(dims, kind)


def const(x):
    return jnp.asarray(x.astype(bf16))


def front(tokens, norm_gain, w_mix_in):
    straight, swapped = first_tables()
    return pl.pallas_call(
        front_kernel,
        out_shape=[
            shape(ROW * A, 128),
            shape(2 * LEN1, 128, kind=f32),
            shape(2 * LEN1, 128, kind=f32),
            shape(2 * LEN1, LEN1),
            shape(2 * LEN1, LEN1),
        ],
        in_specs=[HBM] * 6,
        out_specs=[VMEM] * 5,
        scratch_shapes=[
            pltpu.VMEM((SEQS, A, B, D), bf16),
            pltpu.VMEM((D,), bf16),
            pltpu.VMEM((G, G), bf16),
            pltpu.VMEM((D, F), bf16),
            pltpu.VMEM((32, D), f32),
            pltpu.VMEM((ROW * A, 128), f32),
            pltpu.SemaphoreType.DMA((5,)),
            pltpu.SemaphoreType.DMA((IN_CHUNKS,)),
        ],
        compiler_params=small(16),
        name="front",
    )(
        in_hbm(tokens),
        in_hbm(norm_gain),
        in_hbm(const(channel_table())),
        in_hbm(w_mix_in),
        in_hbm(const(straight)),
        in_hbm(const(swapped)),
    )


def first(z, straight, swapped, cos, sin):
    return pl.pallas_call(
        first_kernel,
        out_shape=shape(COL, 8, 512),
        in_specs=[VMEM] * 5,
        out_specs=VMEM,
        compiler_params=small(8),
        cost_estimate=pl.CostEstimate(flops=10**9, bytes_accessed=10**7, transcendentals=0),
        name="first",
    )(z, straight, swapped, cos, sin)


def second(v):
    return pl.pallas_call(
        second_kernel,
        out_shape=shape(4 * ROW, 128),
        in_specs=[VMEM] * 2,
        out_specs=VMEM,
        scratch_shapes=[pltpu.VMEM((4 * ROW, 128), f32)],
        compiler_params=small(8),
        cost_estimate=pl.CostEstimate(flops=10**4, bytes_accessed=10**4, transcendentals=0),
        name="second",
    )(v, const(second_table()))


def final(x, w_mix_out):
    return pl.pallas_call(
        final_kernel,
        out_shape=shape(SEQS * 16, D),
        in_specs=[VMEM] * 3,
        out_specs=VMEM,
        compiler_params=small(16),
        name="final",
    )(x, const(order_table()), w_mix_out)


def body(tokens, norm_gain, w_mix_in, w_mix_out):
    y, cos, sin, straight, swapped = front(tokens, norm_gain, w_mix_in)
    z = lax.all_to_all(y, "row", split_axis=0, concat_axis=0, tiled=True)
    o = first(z, straight, swapped, cos, sin)
    v = lax.all_to_all(o, "col", split_axis=0, concat_axis=0, tiled=True)
    s = second(v.reshape(2 * LEN2, 512))
    x = lax.all_to_all(s, "row", split_axis=0, concat_axis=0, tiled=True)
    return final(x, w_mix_out).reshape(SEQS, 1, 16, D)


def solution(mesh):
    placed = (P(None, "row", "col", None), P(), P(), P())
    return jax.shard_map(
        body, mesh=mesh, in_specs=placed, out_specs=P(None, "row", "col", None), check_vma=False
    )
```
